32 devices in a mesh: kv: 8 (over z, x), tp: 4 (over y, core).
Axes of the slice: x: 2, y: 2, z: 4, core: 2. Of those that a mesh axis runs over, the one named last changes fastest.
Arguments:
- activations: bfloat16 [384, 2048], P(None, ('kv', 'tp')), may hold values from -6 to 6
- latent_cache: bfloat16 [24, 16384, 288], P(None, 'kv'), may hold values from -6 to 6
- lengths: int32 [24], replicated, may hold values from 4096 to 16352, as said below
- accepted: int32 [24], replicated, may hold values from 0 to 16
- parents: int32 [24, 16], replicated, may hold values from -1 to 14, as said below
- w_query_down: bfloat16 [2048, 512], P(('kv', 'tp')), may hold values from -0.125 to 0.125
- w_key_down: bfloat16 [2048, 288], P(('kv', 'tp')), may hold values from -0.125 to 0.125
- gain_input: bfloat16 [2048], P(('kv', 'tp')), may hold values from 0.099609375 to 1.8984375
- gain_query: bfloat16 [512], replicated, may hold values from 0.099609375 to 1.8984375
- gain_key: bfloat16 [256], replicated, may hold values from 0.099609375 to 1.8984375
- w_query: bfloat16 [512, 16, 288], P(None, 'tp'), as said below
- w_value: bfloat16 [16, 256, 64], replicated, may hold values from -0.375 to 0.375
- w_out: bfloat16 [1024, 2048], P('tp', 'kv'), may hold values from -1 to 1, as said below
- gain_output: bfloat16 [2048], P('kv'), may hold values from 0.099609375 to 1.8984375
Outputs:
- mixed: bfloat16 [384, 2048], P(None, 'kv')
- new_cache: bfloat16 [24, 16384, 288], P(None, 'kv')
The draws below stay inside these ranges and needn't reach their ends.
Inputs may be any that keep to these rules, and one draw needn't show every extreme that they name: One sequence has lengths exactly 16352 and another exactly 4096; which ones varies. accepted is between 0 and 16, so the proposals' positions lie below 16384. `parents`: the parent of proposal i is -1 or a proposal with a smaller index; proposal 0 has parent -1; the proposals of exactly one sequence (which one varies) form a single chain; the other sequences' proposals form general trees. `w_query`: entries are normal with standard deviation (1536)^(-1/2) cut at six standard deviations; in the hidden draw the heads whose index is a multiple of 4 are 48 times larger. `w_out`: entries of order (1024)^(-1/2).
All inputs are finite; a program needn't handle non-finite values.
Results may differ from the reference program's by a relative error of at most 0.0096.
The reference program's roundings to bfloat16 on the way count: a program that leaves them out, or rounds other values in their place, can miss the bound.
Values may be sent and summed in bfloat16 or wider, within the bound.
A program may use at most 192 MiB of HBM per device.

```python
import jax
import jax.numpy as jnp
from jax import lax

D = 2048
HEADS = 16
Q_RANK = 512
KV_RANK = 256
ROPE_DIM = 32
NOPE_DIM = 64
V_DIM = 64
PROPS = 16
SEQS = 24
POS_DEV = 2048
CACHE_LEN = 16384
ROWS = 384
N_KV = 8


def draw_w_query(key, part):
    spread = (3.0 * Q_RANK) ** (-0.5)
    drawn = jnp.clip(jax.random.normal(key, (Q_RANK, HEADS, KV_RANK + ROPE_DIM), jnp.float32), -6.0, 6.0) * spread
    return drawn.astype(jnp.bfloat16)


def draw_w_out(key, part):
    fan_width = HEADS * V_DIM
    spread = float(fan_width) ** (-0.5)
    base_key = jax.random.fold_in(key, 31)
    left_key = jax.random.fold_in(key, 32)
    right_key = jax.random.fold_in(key, 33)
    turn_key = jax.random.fold_in(key, 34)
    base = jnp.clip(jax.random.normal(base_key, (fan_width, D), jnp.float32), -4.0, 4.0) * spread
    left_signs = jnp.where(jax.random.bernoulli(left_key, 0.5, (fan_width,)), 1.0, -1.0).astype(jnp.float32)
    right_signs = jnp.where(jax.random.bernoulli(right_key, 0.5, (D,)), 1.0, -1.0).astype(jnp.float32)
    drawn = base + spread * left_signs[:, None] * right_signs[None, :]
    heading = jnp.where(jax.random.bernoulli(turn_key, 0.5, ()), 1.0, -1.0).astype(jnp.float32)
    column_pos = jnp.arange(D, dtype=jnp.float32) / float(D - 1) - 0.5
    column_scale = jnp.exp(heading * column_pos * jnp.log(3.0))
    drawn = drawn * column_scale[None, :]
    return drawn.astype(jnp.bfloat16)


def draw_lengths(key, part):
    value_key = jax.random.fold_in(key, 11)
    pick_key = jax.random.fold_in(key, 12)
    step_key = jax.random.fold_in(key, 13)
    drawn = jax.random.randint(value_key, (SEQS,), CACHE_LEN // 4, CACHE_LEN - 2 * PROPS + 1)
    seq_ids = jnp.arange(SEQS, dtype=jnp.int32)
    longest = jax.random.randint(pick_key, (), 0, SEQS)
    shortest = (longest + jax.random.randint(step_key, (), 1, SEQS)) % SEQS
    drawn = jnp.where(seq_ids == shortest, CACHE_LEN // 4, drawn)
    drawn = jnp.where(seq_ids == longest, CACHE_LEN - 2 * PROPS, drawn)
    return drawn.astype(jnp.int32)


def draw_parents(key, part):
    link_key = jax.random.fold_in(key, 21)
    pick_key = jax.random.fold_in(key, 22)
    slot_ids = jnp.arange(PROPS, dtype=jnp.int32)
    drawn = jax.random.randint(link_key, (SEQS, PROPS), -1, slot_ids[None, :])
    drawn = jnp.where(slot_ids[None, :] == 0, -1, drawn)
    chain_links = slot_ids - 1
    chained = jax.random.randint(pick_key, (), 0, SEQS)
    chain_seq = (jnp.arange(SEQS, dtype=jnp.int32) == chained)[:, None]
    return jnp.where(chain_seq, chain_links[None, :], drawn).astype(jnp.int32)


def set_ends(result, own_key, least, high):
    place = [jax.random.randint(jax.random.fold_in(own_key, axis), (), 0, length) for axis, length in enumerate(result.shape)]
    main_axis = result.shape.index(max(result.shape))
    neighbour = place[:main_axis] + [(place[main_axis] + 1) % result.shape[main_axis]] + place[main_axis + 1:]
    return result.at[tuple(place)].set(least).at[tuple(neighbour)].set(high)


def levels(own_key, shape, shards, smallest, top_value):
    def one(position, parts):
        draws = jax.random.uniform(jax.random.fold_in(jax.random.fold_in(own_key, 6), position), (parts,), jnp.float32, smallest / len(shards), top_value / len(shards))
        return jnp.repeat(jnp.exp(draws), shape[position] // parts).reshape((-1,) + (1,) * (len(shape) - position - 1))

    level = one(*shards[0])
    for cut in shards[1:]:
        level = level * one(*cut)
    return level


def bell_draw(own_key, shape, deviation, reach, pieces=(), held_as=jnp.bfloat16):
    values = jax.random.normal(own_key, shape, jnp.float32) * deviation
    if len(pieces) > 0:
        values = levels(own_key, shape, pieces, -0.22, 0.18) * values
    return jnp.clip(values, min=-reach, max=reach).astype(held_as)


def setup_inputs(seed: int = 0) -> dict:
    key_of = jax.random.split(jax.random.key(seed), 15)
    activations = bell_draw(key_of[0], (ROWS, D), 1.0, 6.0, ((1, 32),))
    latent_cache = bell_draw(key_of[1], (SEQS, CACHE_LEN, KV_RANK + ROPE_DIM), 1.0, 6.0, ((1, 8),))
    lengths = draw_lengths(jax.random.fold_in(key_of[14], 71), 0)
    accepted = set_ends(jax.random.randint(key_of[3], (SEQS,), 0, PROPS + 1), jax.random.fold_in(key_of[3], 1), 0, PROPS).astype(jnp.int32)
    parents = draw_parents(jax.random.fold_in(key_of[14], 71), 0)
    w_query_down = bell_draw(key_of[5], (D, Q_RANK), D ** -0.5, 0.125, ((0, 32),))
    w_key_down = bell_draw(key_of[6], (D, KV_RANK + ROPE_DIM), D ** -0.5, 0.125, ((0, 32),))
    gain_input = jnp.clip(1.0 + 0.18 * jax.random.normal(key_of[7], (D,), jnp.float32), 0.099609375, 1.8984375).astype(jnp.bfloat16)
    gain_query = jnp.clip(1.0 + 0.18 * jax.random.normal(key_of[8], (Q_RANK,), jnp.float32), 0.099609375, 1.8984375).astype(jnp.bfloat16)
    gain_key = jnp.clip(1.0 + 0.18 * jax.random.normal(key_of[9], (KV_RANK,), jnp.float32), 0.099609375, 1.8984375).astype(jnp.bfloat16)
    w_query = draw_w_query(jax.random.fold_in(key_of[14], 71), 0)
    w_value = bell_draw(key_of[11], (HEADS, KV_RANK, V_DIM), KV_RANK ** -0.5, 0.375)
    w_out = draw_w_out(jax.random.fold_in(key_of[14], 71), 0)
    gain_output = jnp.clip(1.0 + 0.18 * jax.random.normal(key_of[13], (D,), jnp.float32), 0.099609375, 1.8984375).astype(jnp.bfloat16)
    return {"activations": activations, "latent_cache": latent_cache, "lengths": lengths, "accepted": accepted, "parents": parents, "w_query_down": w_query_down, "w_key_down": w_key_down, "gain_input": gain_input, "gain_query": gain_query, "gain_key": gain_key, "w_query": w_query, "w_value": w_value, "w_out": w_out, "gain_output": gain_output}


epsilon = 1e-06
rope_base = 10000.0
score_after_mask = -1e+30

def rotate(component, places):
    half_width = component.shape[-1] // 2
    frequency = rope_base ** (-jnp.arange(half_width, dtype=jnp.float32) / half_width)
    angles = places.astype(jnp.float32)[:, None] * frequency[None, :]
    target_shape = (places.shape[0],) + (1,) * (component.ndim - 2) + (half_width,)
    cosine = jnp.cos(angles).reshape(target_shape)
    sine_part = jnp.sin(angles).reshape(target_shape)
    front_half = component[..., :half_width]
    back_half = component[..., half_width:]
    return jnp.concatenate([front_half * cosine - back_half * sine_part, back_half * cosine + front_half * sine_part], axis=-1)

def normalize(values, scales):
    return values * lax.rsqrt(lax.optimization_barrier(jnp.mean(values * values, axis=-1, keepdims=True)) + epsilon) * scales.astype(jnp.float32)

def ancestry(parents):
    seq_count, prop_count = parents.shape
    slot_ids = jnp.arange(prop_count, dtype=jnp.int32)
    parent_links = (parents[:, :, None] == slot_ids[None, None, :]).astype(jnp.float32)
    identity = jnp.broadcast_to(jnp.eye(prop_count, dtype=jnp.float32), parent_links.shape)
    reached = jnp.minimum(identity + parent_links, 1.0)
    for repeat in range((prop_count - 1).bit_length()):
        reached = jnp.minimum(jnp.einsum('sij,sjk->sik', reached, reached, precision=lax.Precision.HIGHEST), 1.0)
    depths = (lax.optimization_barrier(jnp.sum(reached, axis=-1)) - 1.0).astype(jnp.int32)
    return (reached, depths)

def partial_attend(queries, key_rows, slot_index, onehot, reached, w_value):
    score_scale = (NOPE_DIM + ROPE_DIM) ** (-0.5)
    ancestors = jnp.einsum('sij,snj->sin', reached, onehot, precision=lax.Precision.HIGHEST)
    visible = ((slot_index < 0)[:, None, :] | (ancestors > 0.5))[:, :, None, :]
    scores = jnp.einsum('siha,sna->sihn', queries.astype(jnp.float32), key_rows.astype(jnp.float32), precision=lax.Precision.HIGHEST) * score_scale
    masked = jnp.where(visible, scores, score_after_mask)
    maxima = lax.optimization_barrier(jnp.max(masked, axis=-1))
    weights = jnp.where(visible, jnp.exp(masked - maxima[..., None]), 0.0)
    totals = lax.optimization_barrier(jnp.sum(weights, axis=-1))
    rounded = lax.optimization_barrier(weights.astype(jnp.bfloat16))
    weighted = jnp.einsum('sihn,snk->sihk', rounded.astype(jnp.float32), key_rows[:, :, :KV_RANK].astype(jnp.float32), precision=lax.Precision.HIGHEST)
    value_fraction = lax.optimization_barrier((weighted / jnp.maximum(totals, 1.0)[..., None]).astype(jnp.bfloat16))
    values = jnp.einsum('siha,hav->sihv', value_fraction.astype(jnp.float32), w_value.astype(jnp.float32), precision=lax.Precision.HIGHEST).astype(jnp.bfloat16)
    return (maxima, totals, values)

def combine_parts(maxima, totals, values):
    largest = lax.optimization_barrier(jnp.max(maxima, axis=0))
    shares = totals * jnp.exp(maxima - largest[None])
    summed = lax.optimization_barrier(jnp.sum(shares[..., None] * values.astype(jnp.float32), axis=0))
    return summed / lax.optimization_barrier(jnp.sum(shares, axis=0))[..., None]

def location_rows(seq_cache, rows_of, anchor):
    return lax.dynamic_update_slice(seq_cache, rows_of, (anchor, jnp.int32(0)))

def reference(activations, latent_cache, lengths, accepted, parents, w_query_down, w_key_down, gain_input, gain_query, gain_key, w_query, w_value, w_out, gain_output):
    reached, depths = ancestry(parents)
    filled = lengths + accepted
    places = (filled[:, None] + depths).reshape(-1)
    as_float = activations.astype(jnp.float32)
    scaled = (as_float * gain_input.astype(jnp.float32)).astype(jnp.bfloat16)
    inverse = lax.rsqrt(lax.optimization_barrier(jnp.mean(as_float * as_float, axis=-1, keepdims=True)) + epsilon)
    query_raw = jnp.dot(scaled, w_query_down, preferred_element_type=jnp.float32) * inverse
    key_raw = jnp.dot(scaled, w_key_down, preferred_element_type=jnp.float32) * inverse
    query_low = normalize(query_raw, gain_query).astype(jnp.bfloat16)
    mapped_output = jnp.dot(query_low, w_query.reshape(Q_RANK, -1), preferred_element_type=jnp.float32)
    mapped_output = mapped_output.reshape(ROWS, HEADS, KV_RANK + ROPE_DIM)
    queries = jnp.concatenate([mapped_output[..., :KV_RANK], rotate(mapped_output[..., KV_RANK:], places)], axis=-1).astype(jnp.bfloat16)
    fresh_rows = jnp.concatenate([normalize(key_raw[:, :KV_RANK], gain_key), rotate(key_raw[:, KV_RANK:], places)], axis=-1).astype(jnp.bfloat16)
    fresh_block = fresh_rows.reshape(SEQS, PROPS, KV_RANK + ROPE_DIM)
    updated = jax.vmap(location_rows)(latent_cache, fresh_block, filled)
    queries = lax.optimization_barrier(queries).reshape(SEQS, PROPS, HEADS, KV_RANK + ROPE_DIM)
    keys_all = lax.optimization_barrier(updated)

    def one_block(index_block):
        anchor = index_block * POS_DEV
        key_rows = lax.dynamic_slice_in_dim(keys_all, anchor, POS_DEV, 1)
        locations_held = anchor + jnp.arange(POS_DEV, dtype=jnp.int32)
        slot_index = locations_held[None, :] - filled[:, None]
        onehot = (slot_index[:, :, None] == jnp.arange(PROPS, dtype=jnp.int32)[None, None, :]).astype(jnp.float32)
        return partial_attend(queries, key_rows, slot_index, onehot, reached, w_value)
    maxima, totals, values = lax.map(one_block, jnp.arange(N_KV, dtype=jnp.int32))
    values = lax.optimization_barrier(values)
    attended = combine_parts(maxima, totals, values).astype(jnp.bfloat16).reshape(ROWS, HEADS * V_DIM)
    mixed_raw = jnp.dot(attended, w_out, preferred_element_type=jnp.float32)
    mixed = normalize(mixed_raw, gain_output).astype(jnp.bfloat16)
    return (mixed, updated)
```

```python
import functools

import jax
import jax.numpy as jnp
from jax import lax
from jax.experimental import pallas as pl
from jax.experimental.pallas import tpu as pltpu
from jax.sharding import PartitionSpec as P

NOPE_DIM = 64
LANES = 128

epsilon = 1e-06
rope_base = 10000.0
score_after_mask = -1e30
MESH = pl.DeviceIdType.MESH
HIGHEST = lax.Precision.HIGHEST
VMEM = pl.BlockSpec(memory_space=pltpu.VMEM)


def ancestry(parents):
    seq_count, prop_count = parents.shape
    slot_ids = jnp.arange(prop_count, dtype=jnp.int32)
    parent_links = (parents[:, :, None] == slot_ids[None, None, :]).astype(jnp.bfloat16)
    identity = jnp.broadcast_to(jnp.eye(prop_count, dtype=jnp.bfloat16), parent_links.shape)
    reached = jnp.minimum(identity + parent_links, 1.0)
    for repeat in range((prop_count - 1).bit_length()):
        reached = jnp.minimum(
            jnp.einsum("sij,sjk->sik", reached, reached, preferred_element_type=jnp.float32), 1.0
        ).astype(jnp.bfloat16)
    depths = (jnp.sum(reached.astype(jnp.float32), axis=-1) - 1.0).astype(jnp.int32)
    return (reached, depths)


def dot(a, b, precision=None):
    return jnp.dot(a, b, preferred_element_type=jnp.float32, precision=precision)


def dot_nt(a, b, precision=None):
    return lax.dot_general(
        a, b, (((1,), (1,)), ((), ())), preferred_element_type=jnp.float32, precision=precision
    )


def remote(src, dst, send_sem, recv_sem, device_id):
    return pltpu.make_async_remote_copy(
        src_ref=src,
        dst_ref=dst,
        send_sem=send_sem,
        recv_sem=recv_sem,
        device_id=device_id,
        device_id_type=MESH,
    )


def root_mean(values, count):
    return lax.rsqrt(jnp.sum(values * values, axis=-1, keepdims=True) / count + epsilon)


def compress_kernel(
    n_kv, n_tp, width, q_rank, kv_rank, turn_dim,
    x_ref, w_ref, cos_ref, sin_ref, gain_q_ref, gain_k_ref, out_ref,
    got_x, got_w, part, got_part, all_rows,
    send_x, recv_x, send_w, recv_w, send_p, recv_p, send_a, send_b, recv_a,
):
    me_k, me_t = lax.axis_index("kv"), lax.axis_index("tp")
    barrier = pltpu.get_barrier_semaphore()
    for dk in range(n_kv):
        for dt in range(n_tp):
            if dk or dt:
                pl.semaphore_signal(
                    barrier,
                    inc=1,
                    device_id={"kv": lax.rem(me_k + dk, n_kv), "tp": lax.rem(me_t + dt, n_tp)},
                    device_id_type=MESH,
                )
    pl.semaphore_wait(barrier, n_kv * n_tp - 1)

    sends = []
    features = w_ref.shape[0]
    for d in range(1, n_tp):
        peer = lax.rem(me_t + d, n_tp)
        for src, dst, ss, rs in (
            (x_ref.at[peer], got_x.at[me_t], send_x.at[d], recv_x.at[me_t]),
            (w_ref, got_w.at[me_t], send_w.at[d], recv_w.at[me_t]),
        ):
            copy = remote(src, dst, ss, rs, {"tp": peer})
            copy.start()
            sends.append(copy)

    def term(x, w):
        raw = x[:, features:].astype(jnp.float32)
        return dot(x[:, :features], w), jnp.sum(raw * raw, axis=-1, keepdims=True)

    total, squares = term(x_ref[me_t], w_ref[...])
    for d in range(1, n_tp):
        peer = lax.rem(me_t + d, n_tp)
        remote(x_ref.at[peer], got_x.at[peer], send_x.at[d], recv_x.at[peer], {"tp": peer}).wait_recv()
        remote(w_ref, got_w.at[peer], send_w.at[d], recv_w.at[peer], {"tp": peer}).wait_recv()
        more, more_squares = term(got_x[peer], got_w[peer])
        total, squares = total + more, squares + more_squares
    lane = lax.broadcasted_iota(jnp.int32, total.shape, 1)
    total = jnp.where(lane == width - 1, squares, total)
    each = part.shape[1]
    for j in range(n_kv):
        part[j] = total[j * each : (j + 1) * each]

    for d in range(1, n_kv):
        peer = lax.rem(me_k + d, n_kv)
        copy = remote(part.at[peer], got_part.at[me_k], send_p.at[d], recv_p.at[me_k], {"kv": peer})
        copy.start()
        sends.append(copy)
    summed = part[me_k]
    for d in range(1, n_kv):
        peer = lax.rem(me_k + d, n_kv)
        remote(
            part.at[peer], got_part.at[peer], send_p.at[d], recv_p.at[peer], {"kv": peer}
        ).wait_recv()
        summed = summed + got_part[peer]
    model = n_kv * n_tp * features
    inverse = lax.rsqrt(summed[:, width - 1 : width] / model + epsilon)
    query = summed[:, :q_rank] * inverse
    query = query * root_mean(query, q_rank) * gain_q_ref[...]
    latent = summed[:, q_rank : q_rank + kv_rank] * inverse
    latent = latent * root_mean(latent, kv_rank) * gain_k_ref[...]
    turn = summed[:, q_rank + kv_rank :] * inverse
    tail = turn.shape[1]
    swapped = pltpu.roll(turn, tail - turn_dim, 1)
    turned = turn * cos_ref[...] + swapped * sin_ref[...]
    mine = me_t * n_kv + me_k
    all_rows[mine, :, :q_rank] = query.astype(jnp.bfloat16)
    all_rows[mine, :, q_rank : q_rank + kv_rank] = latent.astype(jnp.bfloat16)
    all_rows[mine, :, q_rank + kv_rank :] = turned.astype(jnp.bfloat16)

    sibling = me_t + 1 - 2 * lax.rem(me_t, 2)
    peers = []
    for dy in range(n_tp // 2):
        for dk in range(n_kv):
            if dy or dk:
                peers.append((lax.rem(me_k + dk, n_kv), lax.rem(me_t + 2 * dy, n_tp)))
    for index, (pk, pt) in enumerate(peers):
        copy = remote(
            all_rows.at[mine], all_rows.at[mine], send_a.at[index], recv_a.at[mine],
            {"kv": pk, "tp": pt},
        )
        copy.start()
        sends.append(copy)

    def pass_on(index, block):
        copy = remote(
            all_rows.at[block], all_rows.at[block], send_b.at[index], recv_a.at[block],
            {"tp": sibling},
        )
        copy.start()
        sends.append(copy)

    pass_on(len(peers), mine)
    for index, (pk, pt) in enumerate(peers):
        block = pt * n_kv + pk
        remote(
            all_rows.at[block], all_rows.at[block], send_a.at[index], recv_a.at[block],
            {"kv": pk, "tp": pt},
        ).wait_recv()
        pass_on(index, block)
    for dy in range(n_tp // 2):
        for dk in range(n_kv):
            block = lax.rem(sibling + 2 * dy, n_tp) * n_kv + lax.rem(me_k + dk, n_kv)
            remote(
                all_rows.at[block], all_rows.at[block], send_b.at[0], recv_a.at[block],
                {"tp": sibling},
            ).wait_recv()
    out_ref[...] = all_rows[...]
    for copy in sends:
        copy.wait_send()


def attend_kernel(
    group, rel_ref, low_ref, wq_ref, cos_ref, sin_ref, reached_ref, fresh_ref, cache_ref,
    out_ref, part_ref, stats_ref, q_main, q_turn,
):
    heads, whole, _ = wq_ref.shape
    turn_dim = q_turn.shape[-1]
    rank = whole - turn_dim
    half = turn_dim // 2
    props = reached_ref.shape[-1]
    seqs = q_main.shape[0]
    span = cache_ref.shape[-1]
    step = pl.program_id(0)
    scale = (NOPE_DIM + turn_dim) ** (-0.5)

    @pl.when(step == 0)
    def _():
        low = low_ref[...]
        for h in range(heads):
            main = dot_nt(low, wq_ref[h, :rank, :])
            front, back = wq_ref[h, rank : rank + half, :], wq_ref[h, rank + half :, :]
            turn = dot_nt(low, jnp.concatenate([front, back], axis=0))
            swapped = dot_nt(low, jnp.concatenate([back, front], axis=0))
            turned = turn * cos_ref[...] + swapped * sin_ref[...]
            rows = slice(h * props, (h + 1) * props)
            q_main[:, rows, :] = main.astype(jnp.bfloat16).reshape(seqs, props, rank)
            q_turn[:, rows, :] = turned.astype(jnp.bfloat16).reshape(seqs, props, turn_dim)

    for g in range(group):
        s = step * group + g
        rel = rel_ref[s]
        out_ref[g] = cache_ref[g]
        first = lax.shift_right_arithmetic(rel, 7)
        for more in range(2):
            chunk = first + more

            @pl.when((chunk >= 0) & (chunk < span // LANES))
            def _():
                start = pl.multiple_of(chunk * LANES, LANES)
                slot = start - rel + lax.broadcasted_iota(jnp.int32, (props, LANES), 1)
                onehot = slot == lax.broadcasted_iota(jnp.int32, (props, LANES), 0)
                placed = dot(fresh_ref[g], onehot.astype(jnp.float32).astype(jnp.bfloat16))
                slots = start - rel + lax.broadcasted_iota(jnp.int32, placed.shape, 1)
                old = out_ref[g, :, pl.ds(start, LANES)].astype(jnp.float32)
                new = jnp.where((slots >= 0) & (slots < props), placed, old)
                out_ref[g, :, pl.ds(start, LANES)] = new.astype(jnp.bfloat16)

        slot = lax.broadcasted_iota(jnp.int32, (props, span), 1) - rel
        onehot = slot == lax.broadcasted_iota(jnp.int32, (props, span), 0)
        ancestors = dot(reached_ref[g], onehot.astype(jnp.float32).astype(jnp.bfloat16))
        bias = jnp.where((slot < 0) | (ancestors > 0.5), 0.0, score_after_mask)
        scores = dot(q_main[s], out_ref[g, :rank, :]) + dot(q_turn[s], out_ref[g, rank:, :])
        masked = scores.reshape(heads, props, span) * scale + bias[None]
        top = jnp.max(masked, axis=-1, keepdims=True)
        weights = jnp.exp(masked - jnp.maximum(top, -1e29))
        totals = jnp.sum(weights, axis=-1, keepdims=True)
        prob = weights.astype(jnp.bfloat16).reshape(heads * props, span)
        weighted = dot_nt(prob, out_ref[g, :rank, :]).reshape(heads, props, rank)
        part = (weighted / jnp.maximum(totals, 1.0)).astype(jnp.bfloat16)
        lane = lax.broadcasted_iota(jnp.int32, (props, LANES), 1)
        stats = jnp.zeros((props, LANES), jnp.float32)
        rows = slice(g * props, (g + 1) * props)
        for h in range(heads):
            part_ref[h, rows, :] = part[h]
            stats = jnp.where(lane == h, top[h], stats)
            stats = jnp.where(lane == heads + h, totals[h], stats)
        stats_ref[rows, :] = stats


def project_kernel(
    n_kv, n_tp,
    part_ref, stats_ref, wv_ref, w_out_ref, gain_ref, out_ref,
    vals, stat, got_vals, got_stat, attended, raw, got_raw, sums, result,
    send_v, recv_v, send_s, recv_s, send_a, recv_a, send_r, recv_r, send_q, recv_q, send_o, recv_o,
):
    me_k, me_t = lax.axis_index("kv"), lax.axis_index("tp")
    heads, _, _ = part_ref.shape
    v_dim = wv_ref.shape[1]
    kv_peers = [lax.rem(me_k + d, n_kv) for d in range(n_kv)]
    tp_peers = [lax.rem(me_t + d, n_tp) for d in range(n_tp)]
    barrier = pltpu.get_barrier_semaphore()
    for peer in kv_peers[1:]:
        pl.semaphore_signal(barrier, inc=1, device_id={"kv": peer}, device_id_type=MESH)
    for peer in tp_peers[1:]:
        pl.semaphore_signal(barrier, inc=1, device_id={"tp": peer}, device_id_type=MESH)
    sends = []

    each = vals.shape[1]
    values = jnp.concatenate([dot_nt(part_ref[h], wv_ref[h]) for h in range(heads)], axis=1)
    for j in range(n_kv):
        vals[j] = values[j * each : (j + 1) * each].astype(jnp.bfloat16)
        stat[j] = stats_ref[j * each : (j + 1) * each, :]
    pl.semaphore_wait(barrier, n_kv + n_tp - 2)

    def exchange(axis, peers, src_of, dst, own, send_sem, recv_sem):
        for d in range(1, len(peers)):
            copy = remote(
                src_of(peers[d]), dst.at[own], send_sem.at[d], recv_sem.at[own], {axis: peers[d]}
            )
            copy.start()
            sends.append(copy)

    def arrived(axis, peers, d, src_of, dst, send_sem, recv_sem):
        remote(
            src_of(peers[d]), dst.at[peers[d]], send_sem.at[d], recv_sem.at[peers[d]],
            {axis: peers[d]},
        ).wait_recv()

    exchange("kv", kv_peers, lambda p: stat.at[p], got_stat, me_k, send_s, recv_s)
    exchange("kv", kv_peers, lambda p: vals.at[p], got_vals, me_k, send_v, recv_v)
    for d in range(1, n_kv):
        arrived("kv", kv_peers, d, lambda p: stat.at[p], got_stat, send_s, recv_s)
    all_stats = [stat[me_k]] + [got_stat[p] for p in kv_peers[1:]]
    largest = all_stats[0]
    for one in all_stats[1:]:
        largest = jnp.maximum(largest, one)
    wide = lax.broadcasted_iota(jnp.int32, (each, heads * v_dim), 1)

    def spread(share):
        out = share[:, 0:1]
        for h in range(1, heads):
            out = jnp.where(wide >= h * v_dim, share[:, h : h + 1], out)
        return jnp.broadcast_to(out, wide.shape)

    summed = None
    for d in range(n_kv):
        one = all_stats[d]
        share = pltpu.roll(one, LANES - heads, 1) * jnp.exp(
            jnp.minimum(one - largest, 0.0)
        )
        share = spread(share)
        if d:
            arrived("kv", kv_peers, d, lambda p: vals.at[p], got_vals, send_v, recv_v)
        block = got_vals[kv_peers[d]] if d else vals[me_k]
        term = share * block.astype(jnp.float32)
        summed = term if summed is None else summed + term
        weight = share if d == 0 else weight + share
    attended[me_k] = (summed / weight).astype(jnp.bfloat16)
    exchange("kv", kv_peers, lambda p: attended.at[me_k], attended, me_k, send_a, recv_a)
    for d in range(1, n_kv):
        arrived("kv", kv_peers, d, lambda p: attended.at[p], attended, send_a, recv_a)

    lines = jnp.concatenate([attended[j].astype(jnp.float32) for j in range(n_kv)], axis=0)
    lines = dot(lines.astype(jnp.bfloat16), w_out_ref[...])
    share_rows = raw.shape[1]
    for t in range(n_tp):
        raw[t] = lines[t * share_rows : (t + 1) * share_rows]
    exchange("tp", tp_peers, lambda p: raw.at[p], got_raw, me_t, send_r, recv_r)
    mixed = raw[me_t]
    for d in range(1, n_tp):
        arrived("tp", tp_peers, d, lambda p: raw.at[p], got_raw, send_r, recv_r)
        mixed = mixed + got_raw[tp_peers[d]]
    cols = mixed.shape[1]
    sums[me_k] = dot_nt(jnp.ones((8, cols), jnp.float32), mixed * mixed, HIGHEST)
    exchange("kv", kv_peers, lambda p: sums.at[me_k], sums, me_k, send_q, recv_q)
    for d in range(1, n_kv):
        arrived("kv", kv_peers, d, lambda p: sums.at[p], sums, send_q, recv_q)
    square = sums[0]
    for j in range(1, n_kv):
        square = square + sums[j]
    norm = lax.rsqrt(square / (cols * n_kv) + epsilon)
    eye = lax.broadcasted_iota(jnp.int32, (share_rows, share_rows), 0) == lax.broadcasted_iota(
        jnp.int32, (share_rows, share_rows), 1
    )
    column = dot_nt(eye.astype(jnp.float32), norm, HIGHEST)
    result[me_t] = (mixed * column[:, 0:1] * gain_ref[...]).astype(jnp.bfloat16)
    exchange("tp", tp_peers, lambda p: result.at[me_t], result, me_t, send_o, recv_o)
    for d in range(1, n_tp):
        arrived("tp", tp_peers, d, lambda p: result.at[p], result, send_o, recv_o)
    out_ref[...] = result[...]
    for copy in sends:
        copy.wait_send()


def up(value, to):
    return -(-value // to) * to


def local(
    n_kv,
    n_tp,
    activations,
    latent_cache,
    lengths,
    accepted,
    parents,
    w_query_down,
    w_key_down,
    gain_input,
    gain_query,
    gain_key,
    w_query,
    w_value,
    w_out,
    gain_output,
):
    bf16, f32 = jnp.bfloat16, jnp.float32
    seqs, props = parents.shape
    rows, features = activations.shape
    heads = w_query.shape[1]
    q_rank, kv_rank = gain_query.shape[0], gain_key.shape[0]
    whole = latent_cache.shape[-1]
    turn_dim = whole - kv_rank
    half = turn_dim // 2
    span = latent_cache.shape[1]
    v_dim = w_value.shape[-1]
    cols = w_out.shape[1]
    n_dev = n_kv * n_tp
    me_k, me_t = lax.axis_index("kv"), lax.axis_index("tp")

    reached, depths = ancestry(parents)
    filled = lengths + accepted
    places = (filled[:, None] + depths).reshape(-1)
    frequency = rope_base ** (-jnp.arange(half, dtype=f32) / half)
    angles = places.astype(f32)[:, None] * frequency[None, :]
    cosine, sine = jnp.cos(angles), jnp.sin(angles)
    cosine = jnp.concatenate([cosine, cosine], axis=1)
    sine = jnp.concatenate([-sine, sine], axis=1)

    few = rows // n_dev
    each = up(few, 16)
    tail = up(2 * turn_dim + 1, LANES)
    width = q_rank + kv_rank + tail

    def own_rows(table):
        mine = lax.dynamic_slice_in_dim(table, (me_t * n_kv + me_k) * few, few, 0)
        return jnp.pad(mine, ((0, each - few), (0, tail - turn_dim)))

    scaled = (activations.astype(f32) * gain_input.astype(f32)).astype(bf16)
    x = jnp.concatenate([scaled, activations], axis=1).reshape(n_dev, few, 2 * features)
    x = jnp.pad(x, ((0, 0), (0, each - few), (0, 0))).reshape(n_tp, n_kv * each, 2 * features)
    w = jnp.concatenate(
        [
            w_query_down,
            w_key_down,
            w_key_down[:, kv_rank + half :],
            w_key_down[:, kv_rank : kv_rank + half],
            jnp.zeros((features, tail - 2 * turn_dim), bf16),
        ],
        axis=1,
    )
    dma = pltpu.SemaphoreType.DMA
    gathered = pl.pallas_call(
        functools.partial(compress_kernel, n_kv, n_tp, width, q_rank, kv_rank, turn_dim),
        name="compress",
        out_shape=jax.ShapeDtypeStruct((n_dev, each, width), bf16),
        in_specs=[VMEM] * 6,
        out_specs=VMEM,
        scratch_shapes=[
            pltpu.VMEM((n_tp, n_kv * each, 2 * features), bf16),
            pltpu.VMEM((n_tp, features, width), bf16),
            pltpu.VMEM((n_kv, each, width), f32),
            pltpu.VMEM((n_kv, each, width), f32),
            pltpu.VMEM((n_dev, each, width), bf16),
            dma((n_tp,)), dma((n_tp,)), dma((n_tp,)), dma((n_tp,)),
            dma((n_kv,)), dma((n_kv,)),
            dma((n_dev,)), dma((n_dev,)), dma((n_dev,)),
        ],
        compiler_params=pltpu.CompilerParams(
            collective_id=0, has_side_effects=True, vmem_limit_bytes=32 * 1024 * 1024
        ),
    )(
        x, w, own_rows(cosine), own_rows(sine),
        gain_query.astype(f32)[None], gain_key.astype(f32)[None],
    )
    gathered = gathered[:, :few].reshape(rows, width)
    query_low = gathered[:, :q_rank]
    fresh = gathered[:, q_rank : q_rank + whole].reshape(seqs, props, whole).transpose(0, 2, 1)

    group = 2 if seqs % 2 == 0 else 1
    fixed = lambda *shape: pl.BlockSpec(shape, lambda i, rel: (0,) * len(shape))
    updated, part, stats = pl.pallas_call(
        functools.partial(attend_kernel, group),
        name="attend",
        out_shape=(
            jax.ShapeDtypeStruct((seqs, whole, span), bf16),
            jax.ShapeDtypeStruct((heads, rows, kv_rank), bf16),
            jax.ShapeDtypeStruct((rows, LANES), f32),
        ),
        grid_spec=pltpu.PrefetchScalarGridSpec(
            num_scalar_prefetch=1,
            grid=(seqs // group,),
            in_specs=[
                fixed(rows, q_rank),
                fixed(heads, whole, q_rank),
                fixed(rows, turn_dim),
                fixed(rows, turn_dim),
                pl.BlockSpec((group, props, props), lambda i, rel: (i, 0, 0)),
                pl.BlockSpec((group, whole, props), lambda i, rel: (i, 0, 0)),
                pl.BlockSpec((group, whole, span), lambda i, rel: (i, 0, 0)),
            ],
            out_specs=[
                pl.BlockSpec((group, whole, span), lambda i, rel: (i, 0, 0)),
                pl.BlockSpec((heads, group * props, kv_rank), lambda i, rel: (0, i, 0)),
                pl.BlockSpec((group * props, LANES), lambda i, rel: (i, 0)),
            ],
            scratch_shapes=[
                pltpu.VMEM((seqs, heads * props, kv_rank), bf16),
                pltpu.VMEM((seqs, heads * props, turn_dim), bf16),
            ],
        ),
        compiler_params=pltpu.CompilerParams(vmem_limit_bytes=48 * 1024 * 1024),
    )(
        filled - me_k * span,
        query_low,
        w_query.transpose(1, 2, 0),
        cosine,
        sine,
        reached,
        fresh,
        latent_cache.transpose(0, 2, 1),
    )

    wv = lax.dynamic_slice_in_dim(w_value.transpose(0, 2, 1), me_t * heads, heads, 0)
    per_kv, per_tp = rows // n_kv, rows // n_tp
    mixed = pl.pallas_call(
        functools.partial(project_kernel, n_kv, n_tp),
        name="project",
        out_shape=jax.ShapeDtypeStruct((n_tp, per_tp, cols), bf16),
        in_specs=[VMEM] * 5,
        out_specs=VMEM,
        scratch_shapes=[
            pltpu.VMEM((n_kv, per_kv, heads * v_dim), bf16),
            pltpu.VMEM((n_kv, per_kv, LANES), f32),
            pltpu.VMEM((n_kv, per_kv, heads * v_dim), bf16),
            pltpu.VMEM((n_kv, per_kv, LANES), f32),
            pltpu.VMEM((n_kv, per_kv, heads * v_dim), bf16),
            pltpu.VMEM((n_tp, per_tp, cols), f32),
            pltpu.VMEM((n_tp, per_tp, cols), f32),
            pltpu.VMEM((n_kv, 8, per_tp), f32),
            pltpu.VMEM((n_tp, per_tp, cols), bf16),
            dma((n_kv,)), dma((n_kv,)), dma((n_kv,)), dma((n_kv,)), dma((n_kv,)), dma((n_kv,)),
            dma((n_tp,)), dma((n_tp,)), dma((n_kv,)), dma((n_kv,)), dma((n_tp,)), dma((n_tp,)),
        ],
        compiler_params=pltpu.CompilerParams(
            collective_id=1, has_side_effects=True, vmem_limit_bytes=32 * 1024 * 1024
        ),
    )(part, stats, wv, w_out, gain_output.astype(f32)[None])
    return (mixed.reshape(rows, cols), updated.transpose(0, 2, 1))


def solution(mesh):
    in_specs = (
        P(None, ("kv", "tp")),
        P(None, "kv", None),
        P(),
        P(),
        P(),
        P(("kv", "tp"), None),
        P(("kv", "tp"), None),
        P(("kv", "tp")),
        P(),
        P(),
        P(None, "tp", None),
        P(),
        P("tp", "kv"),
        P("kv"),
    )
    out_specs = (P(None, "kv"), P(None, "kv", None))
    body = functools.partial(local, mesh.shape["kv"], mesh.shape["tp"])
    return jax.shard_map(body, mesh=mesh, in_specs=in_specs, out_specs=out_specs, check_vma=False)
```

```python
import functools

import jax
import jax.numpy as jnp
from jax import lax
from jax.experimental import pallas as pl
from jax.experimental.pallas import tpu as pltpu
from jax.sharding import PartitionSpec as P

NOPE_DIM = 64
LANES = 128

epsilon = 1e-06
rope_base = 10000.0
score_after_mask = -1e30
MESH = pl.DeviceIdType.MESH
HIGHEST = lax.Precision.HIGHEST
VMEM = pl.BlockSpec(memory_space=pltpu.VMEM)


def ancestry(parents):
    seq_count, prop_count = parents.shape
    slot_ids = jnp.arange(prop_count, dtype=jnp.int32)
    parent_links = (parents[:, :, None] == slot_ids[None, None, :]).astype(jnp.bfloat16)
    identity = jnp.broadcast_to(jnp.eye(prop_count, dtype=jnp.bfloat16), parent_links.shape)
    reached = jnp.minimum(identity + parent_links, 1.0)
    for repeat in range((prop_count - 1).bit_length()):
        reached = jnp.minimum(
            jnp.einsum("sij,sjk->sik", reached, reached, preferred_element_type=jnp.float32), 1.0
        ).astype(jnp.bfloat16)
    depths = (jnp.sum(reached.astype(jnp.float32), axis=-1) - 1.0).astype(jnp.int32)
    return (reached, depths)


def dot(a, b, precision=None):
    return jnp.dot(a, b, preferred_element_type=jnp.float32, precision=precision)


def dot_nt(a, b, precision=None):
    return lax.dot_general(
        a, b, (((1,), (1,)), ((), ())), preferred_element_type=jnp.float32, precision=precision
    )


def remote(src, dst, send_sem, recv_sem, device_id):
    return pltpu.make_async_remote_copy(
        src_ref=src,
        dst_ref=dst,
        send_sem=send_sem,
        recv_sem=recv_sem,
        device_id=device_id,
        device_id_type=MESH,
    )


def root_mean(values, count):
    return lax.rsqrt(jnp.sum(values * values, axis=-1, keepdims=True) / count + epsilon)


def compress_kernel(
    n_kv, n_tp, width, q_rank, kv_rank, turn_dim,
    x_ref, w_ref, cos_ref, sin_ref, gain_q_ref, gain_k_ref, out_ref,
    got_x, got_w, part, got_part, all_rows,
    send_x, recv_x, send_w, recv_w, send_p, recv_p, send_a, send_y, send_b, recv_a,
):
    me_k, me_t = lax.axis_index("kv"), lax.axis_index("tp")
    barrier = pltpu.get_barrier_semaphore()
    for dk in range(n_kv):
        for dt in range(n_tp):
            if dk or dt:
                pl.semaphore_signal(
                    barrier,
                    inc=1,
                    device_id={"kv": lax.rem(me_k + dk, n_kv), "tp": lax.rem(me_t + dt, n_tp)},
                    device_id_type=MESH,
                )
    pl.semaphore_wait(barrier, n_kv * n_tp - 1)

    sends = []
    features = w_ref.shape[0]
    for d in range(1, n_tp):
        peer = lax.rem(me_t + d, n_tp)
        for src, dst, ss, rs in (
            (x_ref.at[peer], got_x.at[me_t], send_x.at[d], recv_x.at[me_t]),
            (w_ref, got_w.at[me_t], send_w.at[d], recv_w.at[me_t]),
        ):
            copy = remote(src, dst, ss, rs, {"tp": peer})
            copy.start()
            sends.append(copy)

    def term(x, w):
        raw = x[:, features:].astype(jnp.float32)
        return dot(x[:, :features], w), jnp.sum(raw * raw, axis=-1, keepdims=True)

    total, squares = term(x_ref[me_t], w_ref[...])
    for d in range(1, n_tp):
        peer = lax.rem(me_t + d, n_tp)
        remote(x_ref.at[peer], got_x.at[peer], send_x.at[d], recv_x.at[peer], {"tp": peer}).wait_recv()
        remote(w_ref, got_w.at[peer], send_w.at[d], recv_w.at[peer], {"tp": peer}).wait_recv()
        more, more_squares = term(got_x[peer], got_w[peer])
        total, squares = total + more, squares + more_squares
    lane = lax.broadcasted_iota(jnp.int32, total.shape, 1)
    total = jnp.where(lane == width - 1, squares, total)
    each = part.shape[1]
    for j in range(n_kv):
        part[j] = total[j * each : (j + 1) * each]

    for d in range(1, n_kv):
        peer = lax.rem(me_k + d, n_kv)
        copy = remote(part.at[peer], got_part.at[me_k], send_p.at[d], recv_p.at[me_k], {"kv": peer})
        copy.start()
        sends.append(copy)
    summed = part[me_k]
    for d in range(1, n_kv):
        peer = lax.rem(me_k + d, n_kv)
        remote(
            part.at[peer], got_part.at[peer], send_p.at[d], recv_p.at[peer], {"kv": peer}
        ).wait_recv()
        summed = summed + got_part[peer]
    model = n_kv * n_tp * features
    inverse = lax.rsqrt(summed[:, width - 1 : width] / model + epsilon)
    query = summed[:, :q_rank] * inverse
    query = query * root_mean(query, q_rank) * gain_q_ref[...]
    latent = summed[:, q_rank : q_rank + kv_rank] * inverse
    latent = latent * root_mean(latent, kv_rank) * gain_k_ref[...]
    turn = summed[:, q_rank + kv_rank :] * inverse
    tail = turn.shape[1]
    swapped = pltpu.roll(turn, tail - turn_dim, 1)
    turned = turn * cos_ref[...] + swapped * sin_ref[...]
    mine = me_t * n_kv + me_k
    all_rows[mine, :, :q_rank] = query.astype(jnp.bfloat16)
    all_rows[mine, :, q_rank : q_rank + kv_rank] = latent.astype(jnp.bfloat16)
    all_rows[mine, :, q_rank + kv_rank :] = turned.astype(jnp.bfloat16)

    sibling = me_t + 1 - 2 * lax.rem(me_t, 2)
    def send(block, sem, device_id):
        copy = remote(all_rows.at[block], all_rows.at[block], sem, recv_a.at[block], device_id)
        copy.start()
        sends.append(copy)

    def landed(block):
        remote(
            all_rows.at[block], all_rows.at[block], send_a.at[0], recv_a.at[block], {"tp": sibling}
        ).wait_recv()

    for dk in range(1, n_kv):
        send(mine, send_a.at[dk], {"kv": lax.rem(me_k + dk, n_kv)})
    for dk in range(n_kv):
        block = me_t * n_kv + lax.rem(me_k + dk, n_kv)
        if dk:
            landed(block)
        for dy in range(1, n_tp // 2):
            send(block, send_y.at[dy * n_kv + dk], {"tp": lax.rem(me_t + 2 * dy, n_tp)})
        send(block, send_b.at[dk], {"tp": sibling})
    for dy in range(1, n_tp // 2):
        for dk in range(n_kv):
            block = lax.rem(me_t + 2 * dy, n_tp) * n_kv + lax.rem(me_k + dk, n_kv)
            landed(block)
            send(block, send_b.at[dy * n_kv + dk], {"tp": sibling})
    for dy in range(n_tp // 2):
        for dk in range(n_kv):
            block = lax.rem(sibling + 2 * dy, n_tp) * n_kv + lax.rem(me_k + dk, n_kv)
            landed(block)
    out_ref[...] = all_rows[...]
    for copy in sends:
        copy.wait_send()


def attend_kernel(
    group, rel_ref, low_ref, wq_ref, cos_ref, sin_ref, reached_ref, fresh_ref, cache_ref,
    out_ref, part_ref, stats_ref, q_main, q_turn, bias,
):
    heads, whole, _ = wq_ref.shape
    turn_dim = q_turn.shape[-1]
    rank = whole - turn_dim
    half = turn_dim // 2
    props = reached_ref.shape[-1]
    seqs = q_main.shape[0]
    span = cache_ref.shape[-1]
    step = pl.program_id(0)
    scale = (NOPE_DIM + turn_dim) ** (-0.5)

    @pl.when(step == 0)
    def _():
        low = low_ref[...]
        for h in range(heads):
            main = dot_nt(low, wq_ref[h, :rank, :])
            front, back = wq_ref[h, rank : rank + half, :], wq_ref[h, rank + half :, :]
            turn = dot_nt(low, jnp.concatenate([front, back], axis=0))
            swapped = dot_nt(low, jnp.concatenate([back, front], axis=0))
            turned = turn * cos_ref[...] + swapped * sin_ref[...]
            rows = slice(h * props, (h + 1) * props)
            q_main[:, rows, :] = main.astype(jnp.bfloat16).reshape(seqs, props, rank)
            q_turn[:, rows, :] = turned.astype(jnp.bfloat16).reshape(seqs, props, turn_dim)

    for g in range(group):
        s = step * group + g
        rel = rel_ref[s]
        out_ref[g] = cache_ref[g]
        past = lax.broadcasted_iota(jnp.int32, (props, span), 1) < rel
        bias[g] = jnp.where(past, 0.0, score_after_mask)
        first = lax.shift_right_arithmetic(rel, 7)
        for more in range(2):
            chunk = first + more

            @pl.when((chunk >= 0) & (chunk < span // LANES))
            def _():
                start = pl.multiple_of(chunk * LANES, LANES)
                slot = start - rel + lax.broadcasted_iota(jnp.int32, (props, LANES), 1)
                onehot = slot == lax.broadcasted_iota(jnp.int32, (props, LANES), 0)
                onehot = onehot.astype(jnp.float32).astype(jnp.bfloat16)
                seen = (slot < 0) | (dot(reached_ref[g], onehot) > 0.5)
                bias[g, :, pl.ds(start, LANES)] = jnp.where(seen, 0.0, score_after_mask)
                placed = lax.dot_general(
                    fresh_ref[g], onehot, (((0,), (0,)), ((), ())),
                    preferred_element_type=jnp.float32,
                )
                slots = start - rel + lax.broadcasted_iota(jnp.int32, placed.shape, 1)
                old = out_ref[g, :, pl.ds(start, LANES)].astype(jnp.float32)
                new = jnp.where((slots >= 0) & (slots < props), placed, old)
                out_ref[g, :, pl.ds(start, LANES)] = new.astype(jnp.bfloat16)

    for g in range(group):
        s = step * group + g
        scores = dot(q_main[s], out_ref[g, :rank, :]) + dot(q_turn[s], out_ref[g, rank:, :])
        masked = scores.reshape(heads, props, span) * scale + bias[g][None]
        top = jnp.max(masked, axis=-1, keepdims=True)
        weights = jnp.exp(masked - jnp.maximum(top, -1e29))
        totals = jnp.sum(weights, axis=-1, keepdims=True)
        prob = weights.astype(jnp.bfloat16).reshape(heads * props, span)
        weighted = dot_nt(prob, out_ref[g, :rank, :]).reshape(heads, props, rank)
        part = (weighted / jnp.maximum(totals, 1.0)).astype(jnp.bfloat16)
        lane = lax.broadcasted_iota(jnp.int32, (props, LANES), 1)
        stats = jnp.zeros((props, LANES), jnp.float32)
        rows = slice(g * props, (g + 1) * props)
        for h in range(heads):
            part_ref[h, rows, :] = part[h]
            stats = jnp.where(lane == h, top[h], stats)
            stats = jnp.where(lane == heads + h, totals[h], stats)
        stats_ref[rows, :] = stats


def project_kernel(
    n_kv, n_tp,
    part_ref, stats_ref, wv_ref, w_out_ref, gain_ref, out_ref,
    vals, stat, got_vals, got_stat, attended, raw, got_raw, sums, result,
    send_v, recv_v, send_s, recv_s, send_a, recv_a, send_r, recv_r, send_q, recv_q, send_o, recv_o,
):
    me_k, me_t = lax.axis_index("kv"), lax.axis_index("tp")
    heads, _, _ = part_ref.shape
    v_dim = wv_ref.shape[1]
    kv_peers = [lax.rem(me_k + d, n_kv) for d in range(n_kv)]
    tp_peers = [lax.rem(me_t + d, n_tp) for d in range(n_tp)]
    barrier = pltpu.get_barrier_semaphore()
    for peer in kv_peers[1:]:
        pl.semaphore_signal(barrier, inc=1, device_id={"kv": peer}, device_id_type=MESH)
    for peer in tp_peers[1:]:
        pl.semaphore_signal(barrier, inc=1, device_id={"tp": peer}, device_id_type=MESH)
    sends = []

    each = vals.shape[1]
    line = lax.broadcasted_iota(jnp.int32, (16, LANES), 0)
    lane = lax.broadcasted_iota(jnp.int32, (16, LANES), 1)
    tops = (line < heads) & (lane == line)
    counts = (line >= 8) & (line < 8 + heads) & (lane == line - 8 + heads)
    pick = jnp.where(tops | counts, 1.0, 0.0)
    values = jnp.concatenate([dot_nt(part_ref[h], wv_ref[h]) for h in range(heads)], axis=1)
    for j in range(n_kv):
        vals[j] = values[j * each : (j + 1) * each].astype(jnp.bfloat16)
        stat[j] = dot_nt(pick, stats_ref[j * each : (j + 1) * each, :], HIGHEST)
    pl.semaphore_wait(barrier, n_kv + n_tp - 2)

    def exchange(axis, peers, src_of, dst, own, send_sem, recv_sem):
        for d in range(1, len(peers)):
            copy = remote(
                src_of(peers[d]), dst.at[own], send_sem.at[d], recv_sem.at[own], {axis: peers[d]}
            )
            copy.start()
            sends.append(copy)

    def arrived(axis, peers, d, src_of, dst, send_sem, recv_sem):
        remote(
            src_of(peers[d]), dst.at[peers[d]], send_sem.at[d], recv_sem.at[peers[d]],
            {axis: peers[d]},
        ).wait_recv()

    exchange("kv", kv_peers, lambda p: stat.at[p], got_stat, me_k, send_s, recv_s)
    exchange("kv", kv_peers, lambda p: vals.at[p], got_vals, me_k, send_v, recv_v)
    for d in range(1, n_kv):
        arrived("kv", kv_peers, d, lambda p: stat.at[p], got_stat, send_s, recv_s)
    all_stats = [stat[me_k]] + [got_stat[p] for p in kv_peers[1:]]
    largest = all_stats[0][:8]
    for one in all_stats[1:]:
        largest = jnp.maximum(largest, one[:8])
    shares = jnp.concatenate([one[8:] * jnp.exp(one[:8] - largest) for one in all_stats], axis=0)
    turn_eye = lax.broadcasted_iota(jnp.int32, (each, each), 0) == lax.broadcasted_iota(
        jnp.int32, (each, each), 1
    )
    shares = dot_nt(turn_eye.astype(jnp.float32), shares, HIGHEST)
    wide = lax.broadcasted_iota(jnp.int32, (each, heads * v_dim), 1)

    def spread(d):
        out = shares[:, 8 * d : 8 * d + 1]
        for h in range(1, heads):
            out = jnp.where(wide >= h * v_dim, shares[:, 8 * d + h : 8 * d + h + 1], out)
        return jnp.broadcast_to(out, wide.shape)

    summed = None
    for d in range(n_kv):
        share = spread(d)
        if d:
            arrived("kv", kv_peers, d, lambda p: vals.at[p], got_vals, send_v, recv_v)
        block = got_vals[kv_peers[d]] if d else vals[me_k]
        term = share * block.astype(jnp.float32)
        summed = term if summed is None else summed + term
        weight = share if d == 0 else weight + share
    attended[me_k] = (summed / weight).astype(jnp.bfloat16)
    exchange("kv", kv_peers, lambda p: attended.at[me_k], attended, me_k, send_a, recv_a)
    for d in range(1, n_kv):
        arrived("kv", kv_peers, d, lambda p: attended.at[p], attended, send_a, recv_a)

    lines = jnp.concatenate([attended[j].astype(jnp.float32) for j in range(n_kv)], axis=0)
    lines = dot(lines.astype(jnp.bfloat16), w_out_ref[...])
    share_rows = raw.shape[1]
    for t in range(n_tp):
        raw[t] = lines[t * share_rows : (t + 1) * share_rows]
    exchange("tp", tp_peers, lambda p: raw.at[p], got_raw, me_t, send_r, recv_r)
    mixed = raw[me_t]
    for d in range(1, n_tp):
        arrived("tp", tp_peers, d, lambda p: raw.at[p], got_raw, send_r, recv_r)
        mixed = mixed + got_raw[tp_peers[d]]
    cols = mixed.shape[1]
    sums[me_k] = dot_nt(jnp.ones((8, cols), jnp.float32), mixed * mixed, HIGHEST)
    exchange("kv", kv_peers, lambda p: sums.at[me_k], sums, me_k, send_q, recv_q)
    for d in range(1, n_kv):
        arrived("kv", kv_peers, d, lambda p: sums.at[p], sums, send_q, recv_q)
    square = sums[0]
    for j in range(1, n_kv):
        square = square + sums[j]
    norm = lax.rsqrt(square / (cols * n_kv) + epsilon)
    eye = lax.broadcasted_iota(jnp.int32, (share_rows, share_rows), 0) == lax.broadcasted_iota(
        jnp.int32, (share_rows, share_rows), 1
    )
    column = dot_nt(eye.astype(jnp.float32), norm, HIGHEST)
    result[me_t] = (mixed * column[:, 0:1] * gain_ref[...]).astype(jnp.bfloat16)
    exchange("tp", tp_peers, lambda p: result.at[me_t], result, me_t, send_o, recv_o)
    for d in range(1, n_tp):
        arrived("tp", tp_peers, d, lambda p: result.at[p], result, send_o, recv_o)
    out_ref[...] = result[...]
    for copy in sends:
        copy.wait_send()


def up(value, to):
    return -(-value // to) * to


def local(
    n_kv,
    n_tp,
    activations,
    latent_cache,
    lengths,
    accepted,
    parents,
    w_query_down,
    w_key_down,
    gain_input,
    gain_query,
    gain_key,
    w_query,
    w_value,
    w_out,
    gain_output,
):
    bf16, f32 = jnp.bfloat16, jnp.float32
    seqs, props = parents.shape
    rows, features = activations.shape
    heads = w_query.shape[1]
    q_rank, kv_rank = gain_query.shape[0], gain_key.shape[0]
    whole = latent_cache.shape[-1]
    turn_dim = whole - kv_rank
    half = turn_dim // 2
    span = latent_cache.shape[1]
    v_dim = w_value.shape[-1]
    cols = w_out.shape[1]
    n_dev = n_kv * n_tp
    me_k, me_t = lax.axis_index("kv"), lax.axis_index("tp")

    reached, depths = ancestry(parents)
    filled = lengths + accepted
    places = (filled[:, None] + depths).reshape(-1)
    frequency = rope_base ** (-jnp.arange(half, dtype=f32) / half)
    angles = places.astype(f32)[:, None] * frequency[None, :]
    cosine, sine = jnp.cos(angles), jnp.sin(angles)
    cosine = jnp.concatenate([cosine, cosine], axis=1)
    sine = jnp.concatenate([-sine, sine], axis=1)

    few = rows // n_dev
    each = up(few, 16)
    tail = up(2 * turn_dim + 1, LANES)
    width = q_rank + kv_rank + tail

    def own_rows(table):
        mine = lax.dynamic_slice_in_dim(table, (me_t * n_kv + me_k) * few, few, 0)
        return jnp.pad(mine, ((0, each - few), (0, tail - turn_dim)))

    scaled = (activations.astype(f32) * gain_input.astype(f32)).astype(bf16)
    x = jnp.concatenate([scaled, activations], axis=1).reshape(n_dev, few, 2 * features)
    x = jnp.pad(x, ((0, 0), (0, each - few), (0, 0))).reshape(n_tp, n_kv * each, 2 * features)
    w = jnp.concatenate(
        [
            w_query_down,
            w_key_down,
            w_key_down[:, kv_rank + half :],
            w_key_down[:, kv_rank : kv_rank + half],
            jnp.zeros((features, tail - 2 * turn_dim), bf16),
        ],
        axis=1,
    )
    dma = pltpu.SemaphoreType.DMA
    gathered = pl.pallas_call(
        functools.partial(compress_kernel, n_kv, n_tp, width, q_rank, kv_rank, turn_dim),
        name="compress",
        out_shape=jax.ShapeDtypeStruct((n_dev, each, width), bf16),
        in_specs=[VMEM] * 6,
        out_specs=VMEM,
        scratch_shapes=[
            pltpu.VMEM((n_tp, n_kv * each, 2 * features), bf16),
            pltpu.VMEM((n_tp, features, width), bf16),
            pltpu.VMEM((n_kv, each, width), f32),
            pltpu.VMEM((n_kv, each, width), f32),
            pltpu.VMEM((n_dev, each, width), bf16),
            dma((n_tp,)), dma((n_tp,)), dma((n_tp,)), dma((n_tp,)),
            dma((n_kv,)), dma((n_kv,)),
            dma((n_kv,)), dma((n_dev,)), dma((n_dev,)), dma((n_dev,)),
        ],
        compiler_params=pltpu.CompilerParams(
            collective_id=0, has_side_effects=True, vmem_limit_bytes=32 * 1024 * 1024
        ),
    )(
        x, w, own_rows(cosine), own_rows(sine),
        gain_query.astype(f32)[None], gain_key.astype(f32)[None],
    )
    gathered = gathered[:, :few].reshape(rows, width)
    query_low = gathered[:, :q_rank]
    fresh = gathered[:, q_rank : q_rank + whole].reshape(seqs, props, whole)

    group = next(g for g in (3, 2, 1) if seqs % g == 0)
    fixed = lambda *shape: pl.BlockSpec(shape, lambda i, rel: (0,) * len(shape))
    updated, part, stats = pl.pallas_call(
        functools.partial(attend_kernel, group),
        name="attend",
        out_shape=(
            jax.ShapeDtypeStruct((seqs, whole, span), bf16),
            jax.ShapeDtypeStruct((heads, rows, kv_rank), bf16),
            jax.ShapeDtypeStruct((rows, LANES), f32),
        ),
        grid_spec=pltpu.PrefetchScalarGridSpec(
            num_scalar_prefetch=1,
            grid=(seqs // group,),
            in_specs=[
                fixed(rows, q_rank),
                fixed(heads, whole, q_rank),
                fixed(rows, turn_dim),
                fixed(rows, turn_dim),
                pl.BlockSpec((group, props, props), lambda i, rel: (i, 0, 0)),
                pl.BlockSpec((group, props, whole), lambda i, rel: (i, 0, 0)),
                pl.BlockSpec((group, whole, span), lambda i, rel: (i, 0, 0)),
            ],
            out_specs=[
                pl.BlockSpec((group, whole, span), lambda i, rel: (i, 0, 0)),
                pl.BlockSpec((heads, group * props, kv_rank), lambda i, rel: (0, i, 0)),
                pl.BlockSpec((group * props, LANES), lambda i, rel: (i, 0)),
            ],
            scratch_shapes=[
                pltpu.VMEM((seqs, heads * props, kv_rank), bf16),
                pltpu.VMEM((seqs, heads * props, turn_dim), bf16),
                pltpu.VMEM((group, props, span), f32),
            ],
        ),
        compiler_params=pltpu.CompilerParams(vmem_limit_bytes=48 * 1024 * 1024),
    )(
        filled - me_k * span,
        query_low,
        w_query.transpose(1, 2, 0),
        cosine,
        sine,
        reached,
        fresh,
        latent_cache.transpose(0, 2, 1),
    )

    wv = lax.dynamic_slice_in_dim(w_value.transpose(0, 2, 1), me_t * heads, heads, 0)
    per_kv, per_tp = rows // n_kv, rows // n_tp
    mixed = pl.pallas_call(
        functools.partial(project_kernel, n_kv, n_tp),
        name="project",
        out_shape=jax.ShapeDtypeStruct((n_tp, per_tp, cols), bf16),
        in_specs=[VMEM] * 5,
        out_specs=VMEM,
        scratch_shapes=[
            pltpu.VMEM((n_kv, per_kv, heads * v_dim), bf16),
            pltpu.VMEM((n_kv, 16, per_kv), f32),
            pltpu.VMEM((n_kv, per_kv, heads * v_dim), bf16),
            pltpu.VMEM((n_kv, 16, per_kv), f32),
            pltpu.VMEM((n_kv, per_kv, heads * v_dim), bf16),
            pltpu.VMEM((n_tp, per_tp, cols), f32),
            pltpu.VMEM((n_tp, per_tp, cols), f32),
            pltpu.VMEM((n_kv, 8, per_tp), f32),
            pltpu.VMEM((n_tp, per_tp, cols), bf16),
            dma((n_kv,)), dma((n_kv,)), dma((n_kv,)), dma((n_kv,)), dma((n_kv,)), dma((n_kv,)),
            dma((n_tp,)), dma((n_tp,)), dma((n_kv,)), dma((n_kv,)), dma((n_tp,)), dma((n_tp,)),
        ],
        compiler_params=pltpu.CompilerParams(
            collective_id=1, has_side_effects=True, vmem_limit_bytes=32 * 1024 * 1024
        ),
    )(part, stats, wv, w_out, gain_output.astype(f32)[None])
    return (mixed.reshape(rows, cols), updated.transpose(0, 2, 1))


def solution(mesh):
    in_specs = (
        P(None, ("kv", "tp")),
        P(None, "kv", None),
        P(),
        P(),
        P(),
        P(("kv", "tp"), None),
        P(("kv", "tp"), None),
        P(("kv", "tp")),
        P(),
        P(),
        P(None, "tp", None),
        P(),
        P("tp", "kv"),
        P("kv"),
    )
    out_specs = (P(None, "kv"), P(None, "kv", None))
    body = functools.partial(local, mesh.shape["kv"], mesh.shape["tp"])
    return jax.shard_map(body, mesh=mesh, in_specs=in_specs, out_specs=out_specs, check_vma=False)
```
